256 devices in a mesh: fs: 16 (over y, x), tp: 16 (over z, core).
Axes of the slice: x: 4, y: 4, z: 8, core: 2. Of those that a mesh axis runs over, the one named last changes fastest.
Arguments:
- tokens: bfloat16 [65536, 1024], P(('fs', 'tp')), may hold values from -6 to 6
- norm_in: float32 [1024], replicated, may hold values from 0.1 to 1.9
- value_weight: bfloat16 [1024, 2816], P('fs', 'tp'), may hold values from -0.1875 to 0.1875
- gate_weight: bfloat16 [1024, 2816], P('fs', 'tp'), may hold values from -0.1875 to 0.1875
- value_taps: float32 [3, 2816], P(None, 'tp'), may hold values from -3 to 3
- gate_taps: float32 [3, 2816], P(None, 'tp'), may hold values from -3 to 3
- down_weight: bfloat16 [2816, 1024], P('tp', 'fs'), may hold values from -0.109375 to 0.109375
- norm_out: float32 [1024], replicated, may hold values from 0.1 to 1.9
Outputs:
- mixed: bfloat16 [65536, 1024], P(('fs', 'tp'))
The draws below stay inside these ranges and needn't reach their ends.
All inputs are finite; a program needn't handle non-finite values.
Results may differ from the reference program's by a relative error of at most 0.02.
Values may be sent and summed in bfloat16 or wider, within the bound.
A program may use at most 64 MiB of HBM per device.

```python
import jax
import jax.numpy as jnp
from jax import lax

D = 1024
FF = 2816
TAPS = 3
TOKENS = 65536


def level_of(key, shape, split, least, high):
    gain = 1.0
    for axis_at, parts in split:
        draws = jax.random.uniform(jax.random.fold_in(jax.random.fold_in(key, 6), axis_at), (parts,), jnp.float32, least / len(split), high / len(split))
        gain = gain * jnp.repeat(jnp.exp(draws), shape[axis_at] // parts).reshape((-1,) + (1,) * (len(shape) - 1 - axis_at))
    return gain


def noise(own_key, dims, deviation, reach, cuts=(), held_as=jnp.bfloat16):
    values = deviation * jax.random.normal(own_key, dims, jnp.float32)
    if cuts:
        values = values * level_of(own_key, dims, cuts, -0.22, 0.18)
    return jnp.clip(values, -reach, reach).astype(held_as)


def setup_inputs(seed: int = 0) -> dict:
    splits = jax.random.split(jax.random.key(seed), 9)
    tokens = noise(splits[0], (TOKENS, D), 1.0, 6.0, ((0, 256),))
    norm_in = jnp.clip(1.0 + 0.18 * jax.random.normal(splits[1], (D,), jnp.float32), 0.1, 1.9)
    value_weight = noise(splits[2], (D, FF), D ** -0.5, 0.1875, ((0, 16), (1, 16)))
    gate_weight = noise(splits[3], (D, FF), D ** -0.5, 0.1875, ((0, 16), (1, 16)))
    value_taps = noise(splits[4], (TAPS, FF), 0.6, 3.0, ((1, 16),), jnp.float32)
    gate_taps = noise(splits[5], (TAPS, FF), 0.6, 3.0, ((1, 16),), jnp.float32)
    down_weight = noise(splits[6], (FF, D), FF ** -0.5, 0.109375, ((0, 16), (1, 16)))
    norm_out = jnp.clip(1.0 + 0.18 * jax.random.normal(splits[7], (D,), jnp.float32), 0.1, 1.9)
    return dict(tokens=tokens, norm_in=norm_in, value_weight=value_weight, gate_weight=gate_weight, value_taps=value_taps, gate_taps=gate_taps, down_weight=down_weight, norm_out=norm_out)


norm_eps = 1e-06

def normalize(values, scale):
    wide = values.astype(jnp.float32)
    power = lax.optimization_barrier(jnp.mean(wide * wide, axis=-1, keepdims=True))
    return (wide * jax.lax.rsqrt(power + norm_eps) * scale).astype(jnp.bfloat16)

def causal_conv(signal, taps):
    length = signal.shape[0]
    padded = jnp.pad(signal.astype(jnp.float32), ((2, 0), (0, 0)))
    result = padded[0:length] * taps[0]
    result = result + padded[1:length + 1] * taps[1]
    result = result + padded[2:length + 2] * taps[2]
    return result

def reference(tokens, norm_in, value_weight, gate_weight, value_taps, gate_taps, down_weight, norm_out):
    normed = normalize(tokens, norm_in)
    value = jnp.dot(normed, value_weight, preferred_element_type=jnp.float32).astype(jnp.bfloat16)
    gate = jnp.dot(normed, gate_weight, preferred_element_type=jnp.float32).astype(jnp.bfloat16)
    conv_value = causal_conv(value, value_taps)
    conv_gate = causal_conv(gate, gate_taps)
    hidden = (jax.nn.gelu(conv_gate, approximate=True) * conv_value).astype(jnp.bfloat16)
    projected = jnp.dot(hidden, down_weight, preferred_element_type=jnp.float32)
    return normalize(projected, norm_out)
```

```python
import functools

import jax
import jax.numpy as jnp
from jax import lax
from jax.experimental import pallas as pl
from jax.experimental.pallas import tpu as pltpu
from jax.sharding import Mesh
from jax.sharding import PartitionSpec as P

FS = ("y", "x")
ALL = ("y", "x", "z", "core")
GATHER = ("y", "x", "z")

norm_eps = 1e-06
HALO = 16
LANES = 128


def packed_up(value, gate):
    tail = value.shape[1] - LANES
    pad = jnp.zeros((value.shape[0], LANES // 2 - tail), value.dtype)
    return jnp.concatenate(
        [value[:, :LANES], gate[:, :LANES], value[:, LANES:], pad, gate[:, LANES:], pad],
        axis=1,
    )


def normalized(wide, scale):
    power = jnp.mean(wide * wide, axis=-1, keepdims=True)
    return wide * lax.rsqrt(power + norm_eps) * scale


def ffn_kernel(tokens_ref, scale_ref, up_ref, down_ref, taps_ref, out_ref, normed, upped):
    step = pl.program_id(0)
    rows = out_ref.shape[0]

    @pl.when(step == 0)
    def _():
        wide = tokens_ref[...].astype(jnp.float32)
        normed[...] = normalized(wide, scale_ref[...]).astype(jnp.bfloat16)
        out_ref[...] = jnp.zeros_like(out_ref)

    weights = up_ref[...].reshape(-1, 3 * LANES)
    upped[...] = jnp.dot(normed[...], weights, preferred_element_type=jnp.float32)
    taps = taps_ref[0]
    conv = upped[pl.ds(HALO - 2, rows), :] * taps[0:1]
    conv = conv + upped[pl.ds(HALO - 1, rows), :] * taps[1:2]
    conv = conv + upped[pl.ds(HALO, rows), :] * taps[2:3]
    last = conv[:, 2 * LANES :]
    main = jax.nn.gelu(conv[:, LANES : 2 * LANES], approximate=True) * conv[:, :LANES]
    rest = jax.nn.gelu(pltpu.roll(last, LANES // 2, 1), approximate=True) * last
    hidden = jnp.concatenate([main, rest], axis=1).astype(jnp.bfloat16)
    half = down_ref.shape[2]
    blocks = down_ref[...].reshape(-1, 2 * half, LANES)
    down = jnp.concatenate([blocks[i] for i in range(blocks.shape[0])], axis=1)
    out_ref[...] += jnp.dot(
        hidden[:, : 2 * half], down, preferred_element_type=jnp.float32
    )


def swapped(value, axis):
    return lax.ppermute(value, axis, [(i, i ^ 1) for i in range(lax.axis_size(axis))])


def shards(
    tokens, norm_in, value_weight, gate_weight, value_taps, gate_taps, down_weight, norm_out
):
    count = lax.axis_size(ALL)
    core = lax.axis_index("core")
    rows = tokens.shape[0]
    halo = lax.ppermute(tokens[-HALO:], ALL, [(i, i + 1) for i in range(count - 1)])
    other = swapped(tokens, "core")
    before = jnp.where(core == 0, halo, swapped(halo, "core"))
    first = jnp.where(core == 0, tokens, other)
    second = jnp.where(core == 0, other, tokens)
    block = jnp.concatenate([before, first, second], axis=0)

    up = packed_up(value_weight, gate_weight)
    up_all = lax.all_gather(up, GATHER)
    groups = count // 2
    depth = lax.axis_size("z")
    up_all = up_all.reshape(groups // depth, depth, *up.shape)

    even = lax.rem(lax.axis_index("x"), 2) == 0
    partner = swapped(down_weight, "x")
    left = jnp.where(even, down_weight, partner)
    right = jnp.where(even, partner, down_weight)
    pair = jnp.concatenate([left, right], axis=1)
    pair = jnp.pad(pair, ((0, 192 - pair.shape[0]), (0, 0)))
    own = jnp.where(even, pair[:96], pair[96:])
    down_all = lax.all_gather(own, GATHER).reshape(groups // depth, depth, *own.shape)

    taps = packed_up(value_taps, gate_taps)
    taps_all = lax.all_gather(taps, "z")

    wide = rows * 2
    spec = pl.BlockSpec
    partial = pl.pallas_call(
        ffn_kernel,
        grid=(depth,),
        in_specs=[
            spec((wide + HALO, tokens.shape[1]), lambda i: (0, 0)),
            spec((1, tokens.shape[1]), lambda i: (0, 0)),
            spec((groups // depth, 1, *up.shape), lambda i: (0, i, 0, 0)),
            spec((groups // depth, 1, *own.shape), lambda i: (0, i, 0, 0)),
            spec((1, *taps.shape), lambda i: (i, 0, 0)),
        ],
        out_specs=spec((wide, tokens.shape[1]), lambda i: (0, 0)),
        out_shape=jax.ShapeDtypeStruct((wide, tokens.shape[1]), jnp.float32),
        scratch_shapes=[
            pltpu.VMEM((wide + HALO, tokens.shape[1]), jnp.bfloat16),
            pltpu.VMEM((wide + HALO, 3 * LANES), jnp.float32),
        ],
        compiler_params=pltpu.CompilerParams(vmem_limit_bytes=48 * 2**20),
        cost_estimate=pl.CostEstimate(
            flops=5 * 10**9, bytes_accessed=12 * 10**6, transcendentals=10**6
        ),
    )(block, norm_in[None], up_all, down_all, taps_all)

    mine = jnp.where(core == 0, partial[:rows], partial[rows:])
    theirs = jnp.where(core == 0, partial[rows:], partial[:rows]).astype(jnp.bfloat16)
    total = mine + swapped(theirs, "core").astype(jnp.float32)
    return normalized(total, norm_out).astype(jnp.bfloat16)


def solution(mesh):
    split = Mesh(mesh.devices.reshape(4, 4, 8, 2), ALL)
    return jax.shard_map(
        shards,
        mesh=split,
        in_specs=(
            P(ALL, None),
            P(),
            P(FS, ("z", "core")),
            P(FS, ("z", "core")),
            P(None, ("z", "core")),
            P(None, ("z", "core")),
            P(("z", "core"), FS),
            P(),
        ),
        out_specs=P(ALL, None),
        check_vma=False,
    )
```

```python
import jax
import jax.numpy as jnp
from jax import lax
from jax.experimental import pallas as pl
from jax.experimental.pallas import tpu as pltpu
from jax.sharding import Mesh
from jax.sharding import PartitionSpec as P

FS = ("y", "x")
ALL = ("y", "x", "z", "core")
MESH = pl.DeviceIdType.MESH
DMA = pltpu.SemaphoreType.DMA

norm_eps = 1e-06
HALO = 16
LANES = 128
NX = NY = 4
NZ = 8
PART = 32


def packed_up(value, gate):
    tail = value.shape[1] - LANES
    pad = jnp.zeros((value.shape[0], LANES // 2 - tail), value.dtype)
    return jnp.concatenate(
        [value[:, :LANES], gate[:, :LANES], value[:, LANES:], pad, gate[:, LANES:], pad],
        axis=1,
    )


def packed_down(down):
    half = 96
    pad = jnp.zeros((2 * half - down.shape[0], down.shape[1]), down.dtype)
    low = jnp.concatenate([down[half:], pad], axis=0)
    return jnp.concatenate([down[:half], low], axis=1)


def normalized(wide, scale):
    power = jnp.mean(wide * wide, axis=-1, keepdims=True)
    return wide * lax.rsqrt(power + norm_eps) * scale


def moved(ref, send, recv, to):
    return pltpu.make_async_remote_copy(
        src_ref=ref, dst_ref=ref, send_sem=send, recv_sem=recv, device_id=to, device_id_type=MESH
    )


def kernel(
    tokens_ref,
    norm_in_ref,
    value_ref,
    gate_ref,
    value_taps_ref,
    gate_taps_ref,
    down_ref,
    norm_out_ref,
    out_ref,
    up_all,
    down_all,
    taps_all,
    rows_all,
    halo,
    normed,
    upped,
    total,
    leaving,
    arriving,
    uz_s, uz_r, tz_s, tz_r,
    ay_s, ay_r, bx_s, bx_r,
    ax_s, ax_r, by_s, by_r,
    dx_s, dx_r, dy_s, dy_r,
    dz_s, dz_r,
    pair_s, pair_r, halo_s, halo_r, sum_s, sum_r,
):
    y, x, z, core = (lax.axis_index(name) for name in ALL)
    rows = out_ref.shape[0]
    x_up, x_down, x_far = (lax.rem(x + k, NX) for k in (1, 3, 2))
    y_up, y_down, y_far = (lax.rem(y + k, NY) for k in (1, 3, 2))
    z_up, z_down = lax.rem(z + 1, NZ), lax.rem(z + NZ - 1, NZ)
    to_xu, to_xd = {"x": x_up}, {"x": x_down}
    to_yu, to_yd = {"y": y_up}, {"y": y_down}
    to_zu, to_zd = {"z": z_up}, {"z": z_down}
    to_pair = {"core": 1 - core}
    z_wrap = (z + 1) // NZ
    x_wrap = (x + z_wrap) // NX
    to_next = {"z": z_up, "x": lax.rem(x + z_wrap, NX), "y": lax.rem(y + x_wrap, NY)}
    z_back = 1 - (z + NZ - 1) // NZ
    x_back = 1 - (x + NX - z_back) // NX
    to_prev = {"z": z_down, "x": lax.rem(x + NX - z_back, NX), "y": lax.rem(y + NY - x_back, NY)}

    up_all[z, y, x] = packed_up(value_ref[...], gate_ref[...])
    down_all[z, y, x] = packed_down(down_ref[...])
    taps_all[z, 0:3] = packed_up(value_taps_ref[...], gate_taps_ref[...])
    rows_all[core] = tokens_ref[...]

    barrier = pltpu.get_barrier_semaphore()
    for device in (to_xu, to_xd, to_yu, to_yd, to_zu, to_zd, to_pair, to_prev):
        pl.semaphore_signal(barrier, inc=1, device_id=device, device_id_type=MESH)
    pl.semaphore_wait(barrier, 8)

    def block(i):
        step = (i + 1) // 2
        return lax.rem(z + NZ + step - 2 * step * lax.rem(i, 2), NZ)

    def uz(i, b, to):
        return [moved(up_all.at[b, y, x], uz_s.at[i], uz_r.at[i], to),
                moved(taps_all.at[b], tz_s.at[i], tz_r.at[i], to)]

    def uz_half(i, b, lo, to):
        half = [moved(up_all.at[b, y, x, pl.ds(lo, PART)], uz_s.at[i], uz_r.at[i], to)]
        return half + ([moved(taps_all.at[b], tz_s.at[i], tz_r.at[i], to)] if lo == 0 else [])

    def first(i, b, yu, yd, xu, xd):
        return [
            moved(up_all.at[b, yu, x, pl.ds(0, PART)], ay_s.at[i, 0], ay_r.at[i, 0], to_yu),
            moved(up_all.at[b, yd, x, pl.ds(0, PART)], ay_s.at[i, 1], ay_r.at[i, 1], to_yd),
            moved(up_all.at[b, y, xu, pl.ds(PART, PART)], bx_s.at[i, 0], bx_r.at[i, 0], to_xu),
            moved(up_all.at[b, y, xd, pl.ds(PART, PART)], bx_s.at[i, 1], bx_r.at[i, 1], to_xd),
        ]

    def first_far(i, b, yu, yd, xu, xd):
        h = PART // 2
        return [
            moved(up_all.at[b, yu, x, pl.ds(0, h)], ay_s.at[i, 2], ay_r.at[i, 2], to_yu),
            moved(up_all.at[b, yd, x, pl.ds(h, h)], ay_s.at[i, 3], ay_r.at[i, 3], to_yd),
            moved(up_all.at[b, y, xu, pl.ds(PART, h)], bx_s.at[i, 2], bx_r.at[i, 2], to_xu),
            moved(up_all.at[b, y, xd, pl.ds(PART + h, h)], bx_s.at[i, 3], bx_r.at[i, 3], to_xd),
        ]

    def last(i, b, yu, yd, xu, xd):
        return [
            moved(up_all.at[b, :, xu, pl.ds(0, PART)], ax_s.at[i, 0], ax_r.at[i, 0], to_xu),
            moved(up_all.at[b, :, xd, pl.ds(0, PART)], ax_s.at[i, 1], ax_r.at[i, 1], to_xd),
            moved(up_all.at[b, yu, :, pl.ds(PART, PART)], by_s.at[i, 0], by_r.at[i, 0], to_yu),
            moved(up_all.at[b, yd, :, pl.ds(PART, PART)], by_s.at[i, 1], by_r.at[i, 1], to_yd),
        ]

    def last_far(i, b, yu, yd, xu, xd):
        lo, hi = pl.ds(0, 2), pl.ds(2, 2)
        return [
            moved(up_all.at[b, lo, xu, pl.ds(0, PART)], ax_s.at[i, 2], ax_r.at[i, 2], to_xu),
            moved(up_all.at[b, hi, xd, pl.ds(0, PART)], ax_s.at[i, 3], ax_r.at[i, 3], to_xd),
            moved(up_all.at[b, yu, lo, pl.ds(PART, PART)], by_s.at[i, 2], by_r.at[i, 2], to_yu),
            moved(up_all.at[b, yd, hi, pl.ds(PART, PART)], by_s.at[i, 3], by_r.at[i, 3], to_yd),
        ]

    own = (y, y, x, x)
    near = (y_down, y_up, x_down, x_up)
    far = (y_far, y_far, x_far, x_far)

    def dx(xu, xd):
        return [moved(down_all.at[z, y, xu], dx_s.at[0], dx_r.at[0], to_xu),
                moved(down_all.at[z, y, xd], dx_s.at[1], dx_r.at[1], to_xd)]

    def dx_far(xu, xd):
        return [moved(down_all.at[z, y, xu, pl.ds(0, 48)], dx_s.at[2], dx_r.at[2], to_xu),
                moved(down_all.at[z, y, xd, pl.ds(48, 48)], dx_s.at[3], dx_r.at[3], to_xd)]

    def dy(yu, yd):
        return [moved(down_all.at[z, yu], dy_s.at[0], dy_r.at[0], to_yu),
                moved(down_all.at[z, yd], dy_s.at[1], dy_r.at[1], to_yd)]

    def dy_far(yu, yd):
        return [moved(down_all.at[z, yu, pl.ds(0, 2)], dy_s.at[2], dy_r.at[2], to_yu),
                moved(down_all.at[z, yd, pl.ds(2, 2)], dy_s.at[3], dy_r.at[3], to_yd)]

    lines = (y, y_down, y_up, y_far)

    def dz(b, i, slot, p, to):
        return moved(down_all.at[b, lines[p]], dz_s.at[i, p], dz_r.at[slot, p], to)

    def start(copies):
        for copy in copies:
            copy.start()

    def landed(copies):
        for copy in copies:
            copy.wait_recv()

    def left(copies):
        for copy in copies:
            copy.wait_send()

    def send_down_line(p):
        dz(z, 1, 1, p, to_zu).start()
        dz(z, 2, 2, p, to_zd).start()

    def pass_up(i):
        b = block(i)

        @pl.when(i < NZ - 1)
        def _():
            landed(uz(i, b, to_zu))

        @pl.when((i < NZ - 3) & (lax.rem(i, 2) == 1))
        def _():
            start(uz(i + 2, b, to_zu))

        @pl.when((i < NZ - 3) & (lax.rem(i, 2) == 0))
        def _():
            start(uz(i + 2, b, to_zd))

        @pl.when(i == NZ - 3)
        def _():
            start(uz_half(i + 2, b, 0, to_zu))

        @pl.when(i == NZ - 2)
        def _():
            start(uz_half(i + 2, b, PART, to_zd))

        @pl.when(i == NZ - 1)
        def _():
            landed(uz_half(i, b, 0, to_zu))
            landed(uz_half(i + 1, b, PART, to_zd))

    def pass_down(s, p):
        for d in (0, 1):
            i = 2 * s - 1 + d
            to = (to_zu, to_zd)[d]
            b = block(i)
            dz(b, i, i, p, to).wait_recv()

            @pl.when(s < 3)
            def _():
                dz(b, i + 2, i + 2, p, to).start()

            if (p < 2) == (d == 0):
                @pl.when(s == 3)
                def _():
                    dz(b, i + 2, NZ - 1, p, to).start()

    def compute(i):
        b = block(i)
        weights = up_all[b].reshape(NY * NX * 2 * PART, 3 * LANES)
        upped[...] = jnp.dot(normed[...], weights, preferred_element_type=jnp.float32)
        taps = taps_all[b]
        lines_of = []
        for yy in range(NY):
            for xx in range(0, NX, 2):
                even, odd = down_all[b, yy, xx], down_all[b, yy, xx + 1]
                half = LANES // 2
                low = jnp.concatenate([even[:, :half], odd[:, :half]], axis=1)
                high = jnp.concatenate([even[:, half:], odd[:, half:]], axis=1)
                lines_of.append(jnp.concatenate([low, high], axis=0))
        down = jnp.concatenate(lines_of, axis=1)
        for part in (0, 1):
            base = part * rows + HALO
            conv = upped[pl.ds(base - 2, rows), :] * taps[0:1]
            conv = conv + upped[pl.ds(base - 1, rows), :] * taps[1:2]
            conv = conv + upped[pl.ds(base, rows), :] * taps[2:3]
            end = conv[:, 2 * LANES :]
            main = jax.nn.gelu(conv[:, LANES : 2 * LANES], approximate=True) * conv[:, :LANES]
            rest = jax.nn.gelu(pltpu.roll(end, LANES // 2, 1), approximate=True) * end
            hidden = jnp.concatenate([main, rest], axis=1).astype(jnp.bfloat16)
            total[part] += jnp.dot(
                hidden[:, : down.shape[0]], down, preferred_element_type=jnp.float32
            )

    start(uz(1, z, to_zu) + uz(2, z, to_zd))
    start(first(0, z, *own))
    start(dx(x, x))
    to_partner = pltpu.make_async_remote_copy(
        src_ref=tokens_ref, dst_ref=rows_all.at[core], send_sem=pair_s, recv_sem=pair_r,
        device_id=to_pair, device_id_type=MESH,
    )
    to_partner.start()
    total[...] = jnp.zeros_like(total)
    pltpu.make_async_remote_copy(
        src_ref=tokens_ref, dst_ref=rows_all.at[1 - core], send_sem=pair_s, recv_sem=pair_r,
        device_id=to_pair, device_id_type=MESH,
    ).wait_recv()
    edge = pltpu.make_async_remote_copy(
        src_ref=rows_all.at[1, pl.ds(rows - HALO, HALO)], dst_ref=halo, send_sem=halo_s,
        recv_sem=halo_r, device_id=to_next, device_id_type=MESH,
    )
    edge.start()

    for i in (1, 2):
        pass_up(jnp.int32(i))
        start(first(i, block(jnp.int32(i)), *own))

    landed(dx(x_down, x_up))
    start(dx_far(x_down, x_up))
    landed(first(0, z, *near))
    start(first_far(0, z, *near))
    scale = norm_in_ref[...]
    for part in (0, 1):
        wide = rows_all[part].astype(jnp.float32)
        normed[pl.ds(HALO + part * rows, rows), :] = normalized(wide, scale).astype(jnp.bfloat16)
    landed(dx_far(x_far, x_far))
    start(dy(y, y))
    send_down_line(0)
    edge.wait_recv()
    origin = (y + x + z) == 0
    before = normalized(halo[...].astype(jnp.float32), scale)
    normed[0:HALO] = jnp.where(origin, 0.0, before).astype(jnp.bfloat16)

    def turn(n, carry):
        @pl.when((n >= 0) & (n + 3 < NZ))
        def _():
            pass_up(n + 3)
            start(first(n + 3, block(n + 3), *own))

        @pl.when(n + 2 < NZ)
        def _():
            landed(first(n + 2, block(n + 2), *near))
            start(first_far(n + 2, block(n + 2), *near))

        @pl.when(n + 1 < NZ)
        def _():
            landed(first_far(n + 1, block(n + 1), *far))
            start(last(n + 1, block(n + 1), *own))

        @pl.when(n == -1)
        def _():
            landed(dy(y_down, y_up))
            start(dy_far(y_down, y_up))
            send_down_line(1)
            send_down_line(2)

        @pl.when(n == 0)
        def _():
            landed(dy_far(y_far, y_far))
            send_down_line(3)

        @pl.when((n >= 1) & (n < NZ - 1))
        def _():
            s = (n + 1) // 2

            @pl.when(lax.rem(n, 2) == 1)
            def _():
                pass_down(s, 0)
                pass_down(s, 1)

            @pl.when(lax.rem(n, 2) == 0)
            def _():
                pass_down(s, 2)
                pass_down(s, 3)

        @pl.when((n >= 0) & (n < NZ))
        def _():
            landed(last(n, block(n), *near))
            start(last_far(n, block(n), *near))

        @pl.when(n == NZ - 1)
        def _():
            for p in range(4):
                dz(block(NZ - 1), NZ - 1 + p // 2, NZ - 1, p, to_zu).wait_recv()

        @pl.when(n >= 1)
        def _():
            landed(last_far(n - 1, block(n - 1), *far))
            compute(n - 1)

        return carry

    lax.fori_loop(-1, NZ + 1, turn, jnp.int32(0))

    pieces = 4
    size = rows // pieces

    def piece(k, ref):
        return pltpu.make_async_remote_copy(
            src_ref=leaving.at[k], dst_ref=ref.at[k], send_sem=sum_s.at[k],
            recv_sem=sum_r.at[k], device_id=to_pair, device_id_type=MESH,
        )

    for k in range(pieces):
        leaving[k] = total[1 - core, pl.ds(k * size, size), :].astype(jnp.bfloat16)
        if k:
            piece(k - 1, arriving).start()
    piece(pieces - 1, arriving).start()
    out_scale = norm_out_ref[...]
    for k in range(pieces):
        piece(k, arriving).wait_recv()
        whole = total[core, pl.ds(k * size, size), :] + arriving[k].astype(jnp.float32)
        out_ref[pl.ds(k * size, size), :] = normalized(whole, out_scale).astype(jnp.bfloat16)

    def drain(i, carry):
        b = block(i)
        left(first(i, b, *own) + first_far(i, b, *near) + last(i, b, *own) + last_far(i, b, *near))
        return carry

    lax.fori_loop(0, NZ, drain, jnp.int32(0))
    for i in range(1, NZ - 1):
        left(uz(i, z, to_zu))
    left(uz_half(NZ - 1, z, 0, to_zu) + uz_half(NZ, z, PART, to_zd))
    left(dx(x, x) + dx_far(x, x) + dy(y, y) + dy_far(y, y))
    for p in range(4):
        for i in range(1, NZ - 1):
            dz(z, i, i, p, to_zu).wait_send()
        dz(z, NZ - 1 + p // 2, NZ - 1, p, to_zu).wait_send()
    to_partner.wait_send()
    edge.wait_send()
    for k in range(pieces):
        piece(k, arriving).wait_send()


def shards(
    tokens, norm_in, value_weight, gate_weight, value_taps, gate_taps, down_weight, norm_out
):
    rows, width = tokens.shape
    bf16, f32 = jnp.bfloat16, jnp.float32
    vmem = pl.BlockSpec(memory_space=pltpu.VMEM)
    return pl.pallas_call(
        kernel,
        in_specs=[vmem] * 8,
        out_specs=vmem,
        out_shape=jax.ShapeDtypeStruct(tokens.shape, tokens.dtype),
        scratch_shapes=[
            pltpu.VMEM((NZ, NY, NX, 2 * PART, 3 * LANES), bf16),
            pltpu.VMEM((NZ, NY, NX, 96, LANES), bf16),
            pltpu.VMEM((NZ, 8, 3 * LANES), f32),
            pltpu.VMEM((2, rows, width), bf16),
            pltpu.VMEM((HALO, width), bf16),
            pltpu.VMEM((2 * rows + HALO, width), bf16),
            pltpu.VMEM((2 * rows + HALO, 3 * LANES), f32),
            pltpu.VMEM((2, rows, width), f32),
            pltpu.VMEM((4, rows // 4, width), bf16),
            pltpu.VMEM((4, rows // 4, width), bf16),
        ]
        + [DMA((NZ + 1,))] * 4
        + [DMA((NZ, 4))] * 8
        + [DMA((4,))] * 4
        + [DMA((NZ + 1, 4)), DMA((NZ, 4))]
        + [DMA] * 4
        + [DMA((4,))] * 2,
        compiler_params=pltpu.CompilerParams(
            collective_id=0, has_side_effects=True, vmem_limit_bytes=56 * 2**20
        ),
    )(
        tokens, norm_in[None], value_weight, gate_weight, value_taps, gate_taps, down_weight,
        norm_out[None],
    )


def solution(mesh):
    split = Mesh(mesh.devices.reshape(NY, NX, NZ, 2), ALL)
    return jax.shard_map(
        shards,
        mesh=split,
        in_specs=(
            P(ALL, None),
            P(),
            P(FS, ("z", "core")),
            P(FS, ("z", "core")),
            P(None, ("z", "core")),
            P(None, ("z", "core")),
            P(("z", "core"), FS),
            P(),
        ),
        out_specs=P(ALL, None),
        check_vma=False,
    )
```

```python
import jax
import jax.numpy as jnp
from jax import lax
from jax.experimental import pallas as pl
from jax.experimental.pallas import tpu as pltpu
from jax.sharding import Mesh
from jax.sharding import PartitionSpec as P

FS = ("y", "x")
ALL = ("y", "x", "z", "core")
MESH = pl.DeviceIdType.MESH
DMA = pltpu.SemaphoreType.DMA

norm_eps = 1e-06
HALO = 16
LANES = 128
NX = NY = 4
NZ = 8
PART = 32


def packed_up(value, gate):
    tail = value.shape[1] - LANES
    pad = jnp.zeros((value.shape[0], LANES // 2 - tail), value.dtype)
    return jnp.concatenate(
        [value[:, :LANES], gate[:, :LANES], value[:, LANES:], pad, gate[:, LANES:], pad],
        axis=1,
    )


def packed_down(down):
    half = 96
    pad = jnp.zeros((2 * half - down.shape[0], down.shape[1]), down.dtype)
    low = jnp.concatenate([down[half:], pad], axis=0)
    return jnp.concatenate([down[:half], low], axis=1)


def normalized(wide, scale):
    power = jnp.mean(wide * wide, axis=-1, keepdims=True)
    return wide * lax.rsqrt(power + norm_eps) * scale


def moved(ref, send, recv, to):
    return pltpu.make_async_remote_copy(
        src_ref=ref, dst_ref=ref, send_sem=send, recv_sem=recv, device_id=to, device_id_type=MESH
    )


def start(*copies):
    for copy in copies:
        copy.start()


def kernel(
    tokens_ref,
    norm_in_ref,
    value_ref,
    gate_ref,
    value_taps_ref,
    gate_taps_ref,
    down_ref,
    norm_out_ref,
    out_ref,
    value_in,
    gate_in,
    down_in,
    up_all,
    down_all,
    taps_all,
    rows_all,
    halo,
    normed,
    upped,
    total,
    leaving,
    arriving,
    first_s, last_s, uz_s, dxy_s, dz_s,
    uz_r, near_r, far_r, last_r, last_far_r, dx_r, dy_r, dz_r,
    load_s, pair_s, pair_r, halo_s, halo_r, sum_s, sum_r,
):
    y, x, z, core = (lax.axis_index(name) for name in ALL)
    rows = out_ref.shape[0]
    x_up, x_down, x_far = (lax.rem(x + k, NX) for k in (1, 3, 2))
    y_up, y_down, y_far = (lax.rem(y + k, NY) for k in (1, 3, 2))
    z_up, z_down = lax.rem(z + 1, NZ), lax.rem(z + NZ - 1, NZ)
    to_xu, to_xd = {"x": x_up}, {"x": x_down}
    to_yu, to_yd = {"y": y_up}, {"y": y_down}
    to_zu, to_zd = {"z": z_up}, {"z": z_down}
    to_pair = {"core": 1 - core}
    z_wrap = (z + 1) // NZ
    x_wrap = (x + z_wrap) // NX
    to_next = {"z": z_up, "x": lax.rem(x + z_wrap, NX), "y": lax.rem(y + x_wrap, NY)}
    z_back = 1 - (z + NZ - 1) // NZ
    x_back = 1 - (x + NX - z_back) // NX
    to_prev = {"z": z_down, "x": lax.rem(x + NX - z_back, NX), "y": lax.rem(y + NY - x_back, NY)}

    barrier = pltpu.get_barrier_semaphore()
    for device in (to_xu, to_xd, to_yu, to_yd, to_zu, to_zd, to_pair, to_prev):
        pl.semaphore_signal(barrier, inc=1, device_id=device, device_id_type=MESH)
    loads = [
        pltpu.make_async_copy(value_ref, value_in, load_s.at[0]),
        pltpu.make_async_copy(gate_ref, gate_in, load_s.at[1]),
        pltpu.make_async_copy(down_ref, down_in, load_s.at[2]),
        pltpu.make_async_copy(tokens_ref, rows_all.at[core], load_s.at[3]),
    ]
    for load in loads:
        load.start()
    taps_all[z, 0:3] = packed_up(value_taps_ref[...], gate_taps_ref[...])
    total[...] = jnp.zeros_like(total)
    for load in loads:
        load.wait()
    up_all[z, y, x] = packed_up(value_in[...], gate_in[...])
    down_all[z, y, x] = packed_down(down_in[...].T)
    pl.semaphore_wait(barrier, 8)

    def block(i):
        step = (i + 1) // 2
        return lax.rem(z + NZ + step - 2 * step * lax.rem(i, 2), NZ)

    lines = (y, y_down, y_up, y_far)
    posts = (x, x_down, x_up, x_far)
    upper, lower = pl.ds(0, PART), pl.ds(PART, PART)

    def landed(ref, sem):
        moved(ref, pair_s, sem, to_pair).wait_recv()

    def left(ref, sem):
        moved(ref, sem, pair_r, to_pair).wait_send()

    def uz(i, b, to):
        start(
            moved(up_all.at[b, y, x], uz_s, uz_r.at[i - 1], to),
            moved(taps_all.at[b], uz_s, uz_r.at[i - 1], to),
        )

    def pass_up(i):
        b = block(i)
        landed(upped.at[pl.ds(0, 40)], uz_r.at[i - 1])

        @pl.when((i < NZ - 3) & (lax.rem(i, 2) == 1))
        def _():
            uz(i + 2, b, to_zu)

        @pl.when((i < NZ - 3) & (lax.rem(i, 2) == 0))
        def _():
            uz(i + 2, b, to_zd)

        @pl.when(i == NZ - 3)
        def _():
            start(
                moved(up_all.at[b, y, x, upper], uz_s, uz_r.at[NZ - 2], to_zu),
                moved(taps_all.at[b], uz_s, uz_r.at[NZ - 2], to_zu),
            )

        @pl.when(i == NZ - 2)
        def _():
            start(moved(up_all.at[b, y, x, lower], uz_s, uz_r.at[NZ - 2], to_zd))

    def first(i, b):
        near = near_r.at[i]
        start(
            moved(up_all.at[b, y, x, upper], first_s, near, to_yu),
            moved(up_all.at[b, y, x, upper], first_s, near, to_yd),
            moved(up_all.at[b, y, x, lower], first_s, near, to_xu),
            moved(up_all.at[b, y, x, lower], first_s, near, to_xd),
        )

    def relay(i, b):
        h = PART // 2
        far = far_r.at[i]
        landed(up_all.at[b, y, pl.ds(0, 2)], near_r.at[i])
        start(
            moved(up_all.at[b, y_down, x, pl.ds(0, h)], first_s, far, to_yu),
            moved(up_all.at[b, y_up, x, pl.ds(h, h)], first_s, far, to_yd),
            moved(up_all.at[b, y, x_down, pl.ds(PART, h)], first_s, far, to_xu),
            moved(up_all.at[b, y, x_up, pl.ds(PART + h, h)], first_s, far, to_xd),
        )

    def last(i, b, p):
        there = last_r.at[i, (p + 1) // 2]
        start(
            moved(up_all.at[b, lines[p], x, upper], last_s, there, to_xu),
            moved(up_all.at[b, y, posts[p], lower], last_s, there, to_yu),
            moved(up_all.at[b, lines[p], x, upper], last_s, there, to_xd),
            moved(up_all.at[b, y, posts[p], lower], last_s, there, to_yd),
        )

    def finish(i, b):
        landed(up_all.at[b, y, x], far_r.at[i])
        for p in (1, 2, 3):
            last(i, b, p)

    def hand_on(i, b, *ps):
        landed(up_all.at[b, y, pl.ds(0, 2 * len(ps))], last_r.at[i, (ps[0] + 1) // 2])
        there = last_far_r.at[i]
        for p in ps:
            px, to_x, py, to_y = (
                (x_down, to_xu, y_down, to_yu) if p < 2 else (x_up, to_xd, y_up, to_yd)
            )
            start(
                moved(up_all.at[b, lines[p], px, upper], last_s, there, to_x),
                moved(up_all.at[b, py, posts[p], lower], last_s, there, to_y),
            )

    def complete(i, b):
        landed(up_all.at[b, 0], last_far_r.at[i])

    def send_down_line(p):
        start(
            moved(down_all.at[z, lines[p]], dz_s, dz_r.at[0, p], to_zu),
            moved(down_all.at[z, lines[p]], dz_s, dz_r.at[0, p], to_zd),
        )

    def pass_down(s, p):
        landed(down_all.at[0, pl.ds(0, 2)], dz_r.at[s - 1, p])
        for d in (0, 1):
            b, to = block(2 * s - 1 + d), (to_zu, to_zd)[d]

            @pl.when(s < 3)
            def _():
                moved(down_all.at[b, lines[p]], dz_s, dz_r.at[s, p], to).start()

            if (p < 2) == (d == 0):
                @pl.when(s == 3)
                def _():
                    moved(down_all.at[b, lines[p]], dz_s, dz_r.at[3, 0], to).start()

    def compute(i):
        b = block(i)
        weights = up_all[b].reshape(NY * NX * 2 * PART, 3 * LANES)
        upped[...] = jnp.dot(normed[...], weights, preferred_element_type=jnp.float32)
        taps = taps_all[b]
        lines_of = []
        for yy in range(NY):
            for xx in range(0, NX, 2):
                even, odd = down_all[b, yy, xx], down_all[b, yy, xx + 1]
                half = LANES // 2
                low = jnp.concatenate([even[:, :half], odd[:, :half]], axis=1)
                high = jnp.concatenate([even[:, half:], odd[:, half:]], axis=1)
                lines_of.append(jnp.concatenate([low, high], axis=0))
        down = jnp.concatenate(lines_of, axis=1)
        for part in (0, 1):
            base = part * rows + HALO
            conv = upped[pl.ds(base - 2, rows), :] * taps[0:1]
            conv = conv + upped[pl.ds(base - 1, rows), :] * taps[1:2]
            conv = conv + upped[pl.ds(base, rows), :] * taps[2:3]
            end = conv[:, 2 * LANES :]
            main = jax.nn.gelu(conv[:, LANES : 2 * LANES], approximate=True) * conv[:, :LANES]
            rest = jax.nn.gelu(pltpu.roll(end, LANES // 2, 1), approximate=True) * end
            hidden = jnp.concatenate([main, rest], axis=1).astype(jnp.bfloat16)
            total[part] += jnp.dot(
                hidden[:, : down.shape[0]], down, preferred_element_type=jnp.float32
            )

    def at(i):
        return jnp.int32(i), block(jnp.int32(i))

    uz(1, z, to_zu)
    uz(2, z, to_zd)
    dx_near, dx_far = dx_r.at[0], dx_r.at[1]
    start(
        moved(down_all.at[z, y, x], dxy_s, dx_near, to_xu),
        moved(down_all.at[z, y, x], dxy_s, dx_near, to_xd),
    )
    first(*at(0))
    own_rows = moved(rows_all.at[core], pair_s, pair_r, to_pair)
    own_rows.start()

    landed(down_all.at[z, y, pl.ds(0, 2)], dx_near)
    start(
        moved(down_all.at[z, y, x_down, pl.ds(0, 48)], dxy_s, dx_far, to_xu),
        moved(down_all.at[z, y, x_up, pl.ds(48, 48)], dxy_s, dx_far, to_xd),
    )
    relay(*at(0))
    last(*at(0), 0)
    landed(rows_all.at[1 - core], pair_r)
    edge = pltpu.make_async_remote_copy(
        src_ref=rows_all.at[1, pl.ds(rows - HALO, HALO)], dst_ref=halo, send_sem=halo_s,
        recv_sem=halo_r, device_id=to_next, device_id_type=MESH,
    )
    edge.start()
    for i in (1, 2):
        pass_up(jnp.int32(i))
        first(*at(i))

    landed(down_all.at[z, y, x], dx_far)
    dy_near, dy_far = dy_r.at[0], dy_r.at[1]
    start(
        moved(down_all.at[z, y], dxy_s, dy_near, to_yu),
        moved(down_all.at[z, y], dxy_s, dy_near, to_yd),
    )
    send_down_line(0)
    finish(*at(0))
    hand_on(*at(0), 0)
    for i in (1, 2):
        relay(*at(i))
        last(*at(i), 0)
    scale = norm_in_ref[...]
    for part in (0, 1):
        wide = rows_all[part].astype(jnp.float32)
        normed[pl.ds(HALO + part * rows, rows), :] = normalized(wide, scale).astype(jnp.bfloat16)
    for i in (3, 4):
        pass_up(jnp.int32(i))
        first(*at(i))
    landed(down_all.at[z, pl.ds(0, 2)], dy_near)
    start(
        moved(down_all.at[z, y_down, pl.ds(0, 2)], dxy_s, dy_far, to_yu),
        moved(down_all.at[z, y_up, pl.ds(2, 2)], dxy_s, dy_far, to_yd),
    )
    send_down_line(1)
    send_down_line(2)
    finish(*at(1))
    hand_on(*at(0), 1, 2)
    edge.wait_recv()
    origin = (y + x + z) == 0
    before = normalized(halo[...].astype(jnp.float32), scale)
    normed[0:HALO] = jnp.where(origin, 0.0, before).astype(jnp.bfloat16)

    def turn(n, carry):
        @pl.when(n + 5 < NZ)
        def _():
            pass_up(n + 5)
            first(n + 5, block(n + 5))

        @pl.when(n + 3 < NZ)
        def _():
            relay(n + 3, block(n + 3))
            last(n + 3, block(n + 3), 0)

        @pl.when(n == 0)
        def _():
            landed(down_all.at[z, 0], dy_far)
            send_down_line(3)

        @pl.when(n + 2 < NZ)
        def _():
            finish(n + 2, block(n + 2))

        @pl.when(n + 1 < NZ)
        def _():
            hand_on(n + 1, block(n + 1), 0)
            hand_on(n + 1, block(n + 1), 1, 2)

        hand_on(n, block(n), 3)

        @pl.when(n < NZ - 2)
        def _():
            s = (n + 2) // 2

            @pl.when(lax.rem(n, 2) == 0)
            def _():
                pass_down(s, 0)
                pass_down(s, 1)

            @pl.when(lax.rem(n, 2) == 1)
            def _():
                pass_down(s, 2)
                pass_down(s, 3)

        @pl.when(n == NZ - 1)
        def _():
            landed(down_all.at[0], dz_r.at[3, 0])

        complete(n, block(n))
        compute(n)
        return carry

    lax.fori_loop(0, NZ, turn, jnp.int32(0))

    pieces = 4
    size = rows // pieces

    def piece(k, ref):
        return pltpu.make_async_remote_copy(
            src_ref=leaving.at[k], dst_ref=ref.at[k], send_sem=sum_s,
            recv_sem=sum_r.at[k], device_id=to_pair, device_id_type=MESH,
        )

    for k in range(pieces):
        leaving[k] = total[1 - core, pl.ds(k * size, size), :].astype(jnp.bfloat16)
        if k:
            piece(k - 1, arriving).start()
    piece(pieces - 1, arriving).start()
    out_scale = norm_out_ref[...]
    for k in range(pieces):
        piece(k, arriving).wait_recv()
        whole = total[core, pl.ds(k * size, size), :] + arriving[k].astype(jnp.float32)
        out_ref[pl.ds(k * size, size), :] = normalized(whole, out_scale).astype(jnp.bfloat16)

    left(up_all.at[pl.ds(0, 6), 0], first_s)
    left(up_all.at[pl.ds(0, 6)], last_s)
    left(upped.at[pl.ds(0, 280)], uz_s)
    left(down_all.at[pl.ds(0, 5), 0, pl.ds(0, 3)], dxy_s)
    left(down_all.at[pl.ds(0, 7)], dz_s)
    own_rows.wait_send()
    edge.wait_send()
    left(leaving, sum_s)


def shards(
    tokens, norm_in, value_weight, gate_weight, value_taps, gate_taps, down_weight, norm_out
):
    rows, width = tokens.shape
    bf16, f32 = jnp.bfloat16, jnp.float32
    vmem = pl.BlockSpec(memory_space=pltpu.VMEM)
    hbm = pl.BlockSpec(memory_space=pl.ANY)
    return pl.pallas_call(
        kernel,
        in_specs=[hbm, vmem, hbm, hbm, vmem, vmem, hbm, vmem],
        out_specs=vmem,
        out_shape=jax.ShapeDtypeStruct(tokens.shape, tokens.dtype),
        scratch_shapes=[
            pltpu.VMEM(value_weight.shape, bf16),
            pltpu.VMEM(value_weight.shape, bf16),
            pltpu.VMEM(down_weight.shape[::-1], bf16),
            pltpu.VMEM((NZ, NY, NX, 2 * PART, 3 * LANES), bf16),
            pltpu.VMEM((NZ, NY, NX, 96, LANES), bf16),
            pltpu.VMEM((NZ, 8, 3 * LANES), f32),
            pltpu.VMEM((2, rows, width), bf16),
            pltpu.VMEM((HALO, width), bf16),
            pltpu.VMEM((2 * rows + HALO, width), bf16),
            pltpu.VMEM((2 * rows + HALO, 3 * LANES), f32),
            pltpu.VMEM((2, rows, width), f32),
            pltpu.VMEM((4, rows // 4, width), bf16),
            pltpu.VMEM((4, rows // 4, width), bf16),
        ]
        + [DMA] * 5
        + [DMA((NZ - 1,))]
        + [DMA((NZ,))] * 2
        + [DMA((NZ, 3)), DMA((NZ,))]
        + [DMA((2,))] * 2
        + [DMA((4, 4)), DMA((4,))]
        + [DMA] * 5
        + [DMA((4,))],
        compiler_params=pltpu.CompilerParams(
            collective_id=0, has_side_effects=True, vmem_limit_bytes=56 * 2**20
        ),
    )(
        tokens, norm_in[None], value_weight, gate_weight, value_taps, gate_taps, down_weight.T,
        norm_out[None],
    )


def solution(mesh):
    split = Mesh(mesh.devices.reshape(NY, NX, NZ, 2), ALL)
    return jax.shard_map(
        shards,
        mesh=split,
        in_specs=(
            P(ALL, None),
            P(),
            P(FS, ("z", "core")),
            P(FS, ("z", "core")),
            P(None, ("z", "core")),
            P(None, ("z", "core")),
            P(("z", "core"), FS),
            P(),
        ),
        out_specs=P(ALL, None),
        check_vma=False,
    )
```

```python
import jax
import jax.numpy as jnp
from jax import lax
from jax.experimental import pallas as pl
from jax.experimental.pallas import tpu as pltpu
from jax.sharding import Mesh
from jax.sharding import PartitionSpec as P

FS = ("y", "x")
ALL = ("y", "x", "z", "core")
MESH = pl.DeviceIdType.MESH
DMA = pltpu.SemaphoreType.DMA

norm_eps = 1e-06
HALO = 16
LANES = 128
NX = NY = 4
NZ = 8
PART = 32


def packed_up(value, gate):
    tail = value.shape[1] - LANES
    pad = jnp.zeros((value.shape[0], LANES // 2 - tail), value.dtype)
    return jnp.concatenate(
        [value[:, :LANES], gate[:, :LANES], value[:, LANES:], pad, gate[:, LANES:], pad],
        axis=1,
    )


def packed_down(down):
    half = 96
    pad = jnp.zeros((2 * half - down.shape[0], down.shape[1]), down.dtype)
    low = jnp.concatenate([down[half:], pad], axis=0)
    return jnp.concatenate([down[:half], low], axis=1)


def normalized(wide, scale):
    power = jnp.mean(wide * wide, axis=-1, keepdims=True)
    return wide * lax.rsqrt(power + norm_eps) * scale


def moved(ref, send, recv, to):
    return pltpu.make_async_remote_copy(
        src_ref=ref, dst_ref=ref, send_sem=send, recv_sem=recv, device_id=to, device_id_type=MESH
    )


def start(*copies):
    for copy in copies:
        copy.start()


def kernel(
    tokens_ref,
    norm_in_ref,
    value_ref,
    gate_ref,
    value_taps_ref,
    gate_taps_ref,
    down_ref,
    norm_out_ref,
    out_ref,
    value_in,
    gate_in,
    down_in,
    up_all,
    down_all,
    taps_all,
    rows_all,
    halo,
    normed,
    upped,
    total,
    leaving,
    arriving,
    first_s, last_s, uz_s, dxy_s, dz_s,
    uz_r, near_r, far_r, last_r, last_far_r, dx_r, dy_r, dz_r,
    load_s, pair_s, pair_r, halo_s, halo_r, sum_s, sum_r,
):
    y, x, z, core = (lax.axis_index(name) for name in ALL)
    rows = out_ref.shape[0]
    x_up, x_down, x_far = (lax.rem(x + k, NX) for k in (1, 3, 2))
    y_up, y_down, y_far = (lax.rem(y + k, NY) for k in (1, 3, 2))
    z_up, z_down = lax.rem(z + 1, NZ), lax.rem(z + NZ - 1, NZ)
    to_xu, to_xd = {"x": x_up}, {"x": x_down}
    to_yu, to_yd = {"y": y_up}, {"y": y_down}
    to_zu, to_zd = {"z": z_up}, {"z": z_down}
    to_pair = {"core": 1 - core}
    z_wrap = (z + 1) // NZ
    x_wrap = (x + z_wrap) // NX
    to_next = {"z": z_up, "x": lax.rem(x + z_wrap, NX), "y": lax.rem(y + x_wrap, NY)}
    z_back = 1 - (z + NZ - 1) // NZ
    x_back = 1 - (x + NX - z_back) // NX
    to_prev = {"z": z_down, "x": lax.rem(x + NX - z_back, NX), "y": lax.rem(y + NY - x_back, NY)}

    barrier = pltpu.get_barrier_semaphore()
    for device in (to_xu, to_xd, to_yu, to_yd, to_zu, to_zd, to_pair, to_prev):
        pl.semaphore_signal(barrier, inc=1, device_id=device, device_id_type=MESH)
    loads = [
        pltpu.make_async_copy(value_ref, value_in, load_s.at[0]),
        pltpu.make_async_copy(gate_ref, gate_in, load_s.at[1]),
        pltpu.make_async_copy(down_ref, down_in, load_s.at[2]),
        pltpu.make_async_copy(tokens_ref, rows_all.at[core], load_s.at[3]),
    ]
    for load in loads:
        load.start()
    taps_all[z, 0:3] = packed_up(value_taps_ref[...], gate_taps_ref[...])
    total[...] = jnp.zeros_like(total)
    for load in loads:
        load.wait()
    up_all[z, y, x] = packed_up(value_in[...], gate_in[...])
    down_all[z, y, x] = packed_down(down_in[...].T)
    pl.semaphore_wait(barrier, 8)

    def block(i):
        step = (i + 1) // 2
        return lax.rem(z + NZ + step - 2 * step * lax.rem(i, 2), NZ)

    lines = (y, y_down, y_up, y_far)
    posts = (x, x_down, x_up, x_far)
    upper, lower = pl.ds(0, PART), pl.ds(PART, PART)

    def landed(ref, sem):
        moved(ref, pair_s, sem, to_pair).wait_recv()

    def left(ref, sem):
        moved(ref, sem, pair_r, to_pair).wait_send()

    def uz(i, b, to):
        start(
            moved(up_all.at[b, y, x], uz_s, uz_r.at[i - 1], to),
            moved(taps_all.at[b], uz_s, uz_r.at[i - 1], to),
        )

    def pass_up(i):
        b = block(i)
        landed(upped.at[pl.ds(0, 40)], uz_r.at[i - 1])

        @pl.when((i < NZ - 3) & (lax.rem(i, 2) == 1))
        def _():
            uz(i + 2, b, to_zu)

        @pl.when((i < NZ - 3) & (lax.rem(i, 2) == 0))
        def _():
            uz(i + 2, b, to_zd)

        @pl.when(i == NZ - 3)
        def _():
            start(
                moved(up_all.at[b, y, x, upper], uz_s, uz_r.at[NZ - 2], to_zu),
                moved(taps_all.at[b], uz_s, uz_r.at[NZ - 2], to_zu),
            )

        @pl.when(i == NZ - 2)
        def _():
            start(moved(up_all.at[b, y, x, lower], uz_s, uz_r.at[NZ - 2], to_zd))

    def first(i, b):
        near = near_r.at[i]
        start(
            moved(up_all.at[b, y, x, upper], first_s, near, to_yu),
            moved(up_all.at[b, y, x, upper], first_s, near, to_yd),
            moved(up_all.at[b, y, x, lower], first_s, near, to_xu),
            moved(up_all.at[b, y, x, lower], first_s, near, to_xd),
        )

    def relay(i, b):
        h = PART // 2
        far = far_r.at[i]
        landed(up_all.at[b, y, pl.ds(0, 2)], near_r.at[i])
        start(
            moved(up_all.at[b, y_down, x, pl.ds(0, h)], first_s, far, to_yu),
            moved(up_all.at[b, y_up, x, pl.ds(h, h)], first_s, far, to_yd),
            moved(up_all.at[b, y, x_down, pl.ds(PART, h)], first_s, far, to_xu),
            moved(up_all.at[b, y, x_up, pl.ds(PART + h, h)], first_s, far, to_xd),
        )

    def last(i, b, p):
        there = last_r.at[i, (p + 1) // 2]
        start(
            moved(up_all.at[b, lines[p], x, upper], last_s, there, to_xu),
            moved(up_all.at[b, y, posts[p], lower], last_s, there, to_yu),
            moved(up_all.at[b, lines[p], x, upper], last_s, there, to_xd),
            moved(up_all.at[b, y, posts[p], lower], last_s, there, to_yd),
        )

    def finish(i, b):
        landed(up_all.at[b, y, x], far_r.at[i])
        for p in (1, 2, 3):
            last(i, b, p)

    def hand_on(i, b, *ps):
        landed(up_all.at[b, y, pl.ds(0, 2 * len(ps))], last_r.at[i, (ps[0] + 1) // 2])
        there = last_far_r.at[i]
        for p in ps:
            px, to_x, py, to_y = (
                (x_down, to_xu, y_down, to_yu) if p < 2 else (x_up, to_xd, y_up, to_yd)
            )
            start(
                moved(up_all.at[b, lines[p], px, upper], last_s, there, to_x),
                moved(up_all.at[b, py, posts[p], lower], last_s, there, to_y),
            )

    def complete(i, b):
        landed(up_all.at[b, 0], last_far_r.at[i])

    def send_down_line(p):
        start(
            moved(down_all.at[z, lines[p]], dz_s, dz_r.at[0, p], to_zu),
            moved(down_all.at[z, lines[p]], dz_s, dz_r.at[0, p], to_zd),
        )

    def pass_down(s, p):
        landed(down_all.at[0, pl.ds(0, 2)], dz_r.at[s - 1, p])
        for d in (0, 1):
            b, to = block(2 * s - 1 + d), (to_zu, to_zd)[d]

            @pl.when(s < 3)
            def _():
                moved(down_all.at[b, lines[p]], dz_s, dz_r.at[s, p], to).start()

            if (p < 2) == (d == 0):
                @pl.when(s == 3)
                def _():
                    moved(down_all.at[b, lines[p]], dz_s, dz_r.at[3, 0], to).start()

    def compute(i):
        b = block(i)
        weights = up_all[b].reshape(NY * NX * 2 * PART, 3 * LANES)
        upped[...] = jnp.dot(normed[...], weights, preferred_element_type=jnp.float32)
        taps = taps_all[b]
        lines_of = []
        for yy in range(NY):
            for xx in range(0, NX, 2):
                even, odd = down_all[b, yy, xx], down_all[b, yy, xx + 1]
                half = LANES // 2
                low = jnp.concatenate([even[:, :half], odd[:, :half]], axis=1)
                high = jnp.concatenate([even[:, half:], odd[:, half:]], axis=1)
                lines_of.append(jnp.concatenate([low, high], axis=0))
        down = jnp.concatenate(lines_of, axis=1)
        for part in (0, 1):
            base = part * rows + HALO
            conv = upped[pl.ds(base - 2, rows), :] * taps[0:1]
            conv = conv + upped[pl.ds(base - 1, rows), :] * taps[1:2]
            conv = conv + upped[pl.ds(base, rows), :] * taps[2:3]
            end = conv[:, 2 * LANES :]
            main = jax.nn.gelu(conv[:, LANES : 2 * LANES], approximate=True) * conv[:, :LANES]
            rest = jax.nn.gelu(pltpu.roll(end, LANES // 2, 1), approximate=True) * end
            hidden = jnp.concatenate([main, rest], axis=1).astype(jnp.bfloat16)
            total[part] += jnp.dot(
                hidden[:, : down.shape[0]], down, preferred_element_type=jnp.float32
            )

    uz(1, z, to_zu)
    uz(2, z, to_zd)
    dx_near, dx_far = dx_r.at[0], dx_r.at[1]
    start(
        moved(down_all.at[z, y, x], dxy_s, dx_near, to_xu),
        moved(down_all.at[z, y, x], dxy_s, dx_near, to_xd),
    )
    first(jnp.int32(0), z)
    own_rows = moved(rows_all.at[core], pair_s, pair_r, to_pair)
    own_rows.start()
    edge = pltpu.make_async_remote_copy(
        src_ref=rows_all.at[1, pl.ds(rows - HALO, HALO)], dst_ref=halo, send_sem=halo_s,
        recv_sem=halo_r, device_id=to_next, device_id_type=MESH,
    )
    dy_near, dy_far = dy_r.at[0], dy_r.at[1]

    def normalize_rows():
        scale = norm_in_ref[...]
        for part in (0, 1):
            wide = rows_all[part].astype(jnp.float32)
            value = normalized(wide, scale).astype(jnp.bfloat16)
            normed[pl.ds(HALO + part * rows, rows), :] = value

    def normalize_halo():
        edge.wait_recv()
        origin = (y + x + z) == 0
        before = normalized(halo[...].astype(jnp.float32), norm_in_ref[...])
        normed[0:HALO] = jnp.where(origin, 0.0, before).astype(jnp.bfloat16)

    def turn(n, carry):
        @pl.when(n == -4)
        def _():
            landed(down_all.at[z, y, pl.ds(0, 2)], dx_near)
            start(
                moved(down_all.at[z, y, x_down, pl.ds(0, 48)], dxy_s, dx_far, to_xu),
                moved(down_all.at[z, y, x_up, pl.ds(48, 48)], dxy_s, dx_far, to_xd),
            )
            pass_up(n + 5)
            first(n + 5, block(n + 5))

        @pl.when(n == -3)
        def _():
            landed(down_all.at[z, y, x], dx_far)
            start(
                moved(down_all.at[z, y], dxy_s, dy_near, to_yu),
                moved(down_all.at[z, y], dxy_s, dy_near, to_yd),
            )
            send_down_line(0)

        @pl.when(n == -2)
        def _():
            landed(down_all.at[z, pl.ds(0, 2)], dy_near)
            start(
                moved(down_all.at[z, y_down, pl.ds(0, 2)], dxy_s, dy_far, to_yu),
                moved(down_all.at[z, y_up, pl.ds(2, 2)], dxy_s, dy_far, to_yd),
            )
            send_down_line(1)
            send_down_line(2)

        @pl.when(n == -1)
        def _():
            landed(down_all.at[z, 0], dy_far)
            send_down_line(3)

        @pl.when(n + 6 < NZ)
        def _():
            pass_up(n + 6)
            first(n + 6, block(n + 6))

        @pl.when(n + 4 < NZ)
        def _():
            relay(n + 4, block(n + 4))

        @pl.when((n >= -1) & (n + 1 < NZ))
        def _():
            hand_on(n + 1, block(n + 1), 1, 2)
            hand_on(n + 1, block(n + 1), 3)

        @pl.when((n >= -2) & (n + 2 < NZ))
        def _():
            hand_on(n + 2, block(n + 2), 0)

        @pl.when((n >= -3) & (n + 3 < NZ))
        def _():
            finish(n + 3, block(n + 3))

        @pl.when(n + 4 < NZ)
        def _():
            last(n + 4, block(n + 4), 0)

        @pl.when(n == -4)
        def _():
            landed(rows_all.at[1 - core], pair_r)
            edge.start()
            normalize_rows()

        @pl.when(n == -1)
        def _():
            normalize_halo()

        @pl.when((n >= 0) & (n < NZ - 2))
        def _():
            s = (n + 2) // 2

            @pl.when(lax.rem(n, 2) == 0)
            def _():
                pass_down(s, 0)
                pass_down(s, 1)

            @pl.when(lax.rem(n, 2) == 1)
            def _():
                pass_down(s, 2)
                pass_down(s, 3)

        @pl.when(n == NZ - 1)
        def _():
            landed(down_all.at[0], dz_r.at[3, 0])

        @pl.when(n >= 0)
        def _():
            complete(n, block(n))
            compute(n)

        return carry

    lax.fori_loop(-4, NZ, turn, jnp.int32(0))

    pieces = 4
    size = rows // pieces

    def piece(k, ref):
        return pltpu.make_async_remote_copy(
            src_ref=leaving.at[k], dst_ref=ref.at[k], send_sem=sum_s,
            recv_sem=sum_r.at[k], device_id=to_pair, device_id_type=MESH,
        )

    for k in range(pieces):
        leaving[k] = total[1 - core, pl.ds(k * size, size), :].astype(jnp.bfloat16)
        if k:
            piece(k - 1, arriving).start()
    piece(pieces - 1, arriving).start()
    out_scale = norm_out_ref[...]
    for k in range(pieces):
        piece(k, arriving).wait_recv()
        whole = total[core, pl.ds(k * size, size), :] + arriving[k].astype(jnp.float32)
        out_ref[pl.ds(k * size, size), :] = normalized(whole, out_scale).astype(jnp.bfloat16)

    left(up_all.at[pl.ds(0, 6), 0], first_s)
    left(up_all.at[pl.ds(0, 6)], last_s)
    left(upped.at[pl.ds(0, 280)], uz_s)
    left(down_all.at[pl.ds(0, 5), 0, pl.ds(0, 3)], dxy_s)
    left(down_all.at[pl.ds(0, 7)], dz_s)
    own_rows.wait_send()
    edge.wait_send()
    left(leaving, sum_s)


def shards(
    tokens, norm_in, value_weight, gate_weight, value_taps, gate_taps, down_weight, norm_out
):
    rows, width = tokens.shape
    bf16, f32 = jnp.bfloat16, jnp.float32
    vmem = pl.BlockSpec(memory_space=pltpu.VMEM)
    hbm = pl.BlockSpec(memory_space=pl.ANY)
    return pl.pallas_call(
        kernel,
        in_specs=[hbm, vmem, hbm, hbm, vmem, vmem, hbm, vmem],
        out_specs=vmem,
        out_shape=jax.ShapeDtypeStruct(tokens.shape, tokens.dtype),
        scratch_shapes=[
            pltpu.VMEM(value_weight.shape, bf16),
            pltpu.VMEM(value_weight.shape, bf16),
            pltpu.VMEM(down_weight.shape[::-1], bf16),
            pltpu.VMEM((NZ, NY, NX, 2 * PART, 3 * LANES), bf16),
            pltpu.VMEM((NZ, NY, NX, 96, LANES), bf16),
            pltpu.VMEM((NZ, 8, 3 * LANES), f32),
            pltpu.VMEM((2, rows, width), bf16),
            pltpu.VMEM((HALO, width), bf16),
            pltpu.VMEM((2 * rows + HALO, width), bf16),
            pltpu.VMEM((2 * rows + HALO, 3 * LANES), f32),
            pltpu.VMEM((2, rows, width), f32),
            pltpu.VMEM((4, rows // 4, width), bf16),
            pltpu.VMEM((4, rows // 4, width), bf16),
        ]
        + [DMA] * 5
        + [DMA((NZ - 1,))]
        + [DMA((NZ,))] * 2
        + [DMA((NZ, 3)), DMA((NZ,))]
        + [DMA((2,))] * 2
        + [DMA((4, 4)), DMA((4,))]
        + [DMA] * 5
        + [DMA((4,))],
        compiler_params=pltpu.CompilerParams(
            collective_id=0, has_side_effects=True, vmem_limit_bytes=56 * 2**20
        ),
    )(
        tokens, norm_in[None], value_weight, gate_weight, value_taps, gate_taps, down_weight.T,
        norm_out[None],
    )


def solution(mesh):
    split = Mesh(mesh.devices.reshape(NY, NX, NZ, 2), ALL)
    return jax.shard_map(
        shards,
        mesh=split,
        in_specs=(
            P(ALL, None),
            P(),
            P(FS, ("z", "core")),
            P(FS, ("z", "core")),
            P(None, ("z", "core")),
            P(None, ("z", "core")),
            P(("z", "core"), FS),
            P(),
        ),
        out_specs=P(ALL, None),
        check_vma=False,
    )
```

```python
import jax
import jax.numpy as jnp
from jax import lax
from jax.experimental import pallas as pl
from jax.experimental.pallas import tpu as pltpu
from jax.sharding import Mesh
from jax.sharding import PartitionSpec as P

FS = ("y", "x")
ALL = ("y", "x", "z", "core")
MESH = pl.DeviceIdType.MESH
DMA = pltpu.SemaphoreType.DMA

norm_eps = 1e-06
HALO = 16
LANES = 128
NX = NY = 4
NZ = 8
PART = 32


def packed_up(value, gate):
    tail = value.shape[1] - LANES
    pad = jnp.zeros((value.shape[0], LANES // 2 - tail), value.dtype)
    return jnp.concatenate(
        [value[:, :LANES], gate[:, :LANES], value[:, LANES:], pad, gate[:, LANES:], pad],
        axis=1,
    )


def packed_down(down):
    half = 96
    pad = jnp.zeros((2 * half - down.shape[0], down.shape[1]), down.dtype)
    low = jnp.concatenate([down[half:], pad], axis=0)
    return jnp.concatenate([down[:half], low], axis=1)


def normalized(wide, scale):
    power = jnp.mean(wide * wide, axis=-1, keepdims=True)
    return wide * lax.rsqrt(power + norm_eps) * scale


def moved(ref, send, recv, to):
    return pltpu.make_async_remote_copy(
        src_ref=ref, dst_ref=ref, send_sem=send, recv_sem=recv, device_id=to, device_id_type=MESH
    )


def start(*copies):
    for copy in copies:
        copy.start()


def kernel(
    tokens_ref,
    norm_in_ref,
    value_ref,
    gate_ref,
    value_taps_ref,
    gate_taps_ref,
    down_ref,
    norm_out_ref,
    out_ref,
    value_in,
    gate_in,
    down_in,
    up_all,
    down_all,
    taps_all,
    rows_all,
    halo,
    normed,
    upped,
    total,
    leaving,
    arriving,
    first_s, last_s, uz_s, dxy_s, dz_s,
    uz_r, near_r, far_r, last_r, last_far_r, dx_r, dy_r, dz_r,
    load_s, pair_s, pair_r, halo_s, halo_r, sum_s, sum_r,
):
    y, x, z, core = (lax.axis_index(name) for name in ALL)
    rows = out_ref.shape[0]
    x_up, x_down, x_far = (lax.rem(x + k, NX) for k in (1, 3, 2))
    y_up, y_down, y_far = (lax.rem(y + k, NY) for k in (1, 3, 2))
    z_up, z_down = lax.rem(z + 1, NZ), lax.rem(z + NZ - 1, NZ)
    to_xu, to_xd = {"x": x_up}, {"x": x_down}
    to_yu, to_yd = {"y": y_up}, {"y": y_down}
    to_zu, to_zd = {"z": z_up}, {"z": z_down}
    to_pair = {"core": 1 - core}
    z_wrap = (z + 1) // NZ
    x_wrap = (x + z_wrap) // NX
    to_next = {"z": z_up, "x": lax.rem(x + z_wrap, NX), "y": lax.rem(y + x_wrap, NY)}
    z_back = 1 - (z + NZ - 1) // NZ
    x_back = 1 - (x + NX - z_back) // NX
    to_prev = {"z": z_down, "x": lax.rem(x + NX - z_back, NX), "y": lax.rem(y + NY - x_back, NY)}

    barrier = pltpu.get_barrier_semaphore()
    for device in (to_xu, to_xd, to_yu, to_yd, to_zu, to_zd, to_pair, to_prev):
        pl.semaphore_signal(barrier, inc=1, device_id=device, device_id_type=MESH)
    loads = [
        pltpu.make_async_copy(value_ref, value_in, load_s.at[0]),
        pltpu.make_async_copy(gate_ref, gate_in, load_s.at[1]),
        pltpu.make_async_copy(down_ref, down_in, load_s.at[2]),
        pltpu.make_async_copy(tokens_ref, rows_all.at[core], load_s.at[3]),
    ]
    for load in loads:
        load.start()
    taps_all[z, 0:3] = packed_up(value_taps_ref[...], gate_taps_ref[...])
    total[...] = jnp.zeros_like(total)
    for load in loads:
        load.wait()
    up_all[z, y, x] = packed_up(value_in[...], gate_in[...])
    down_all[z, y, x] = packed_down(down_in[...].T)
    pl.semaphore_wait(barrier, 8)

    def block(i):
        step = (i + 1) // 2
        return lax.rem(z + NZ + step - 2 * step * lax.rem(i, 2), NZ)

    lines = (y, y_down, y_up, y_far)
    posts = (x, x_down, x_up, x_far)
    upper, lower = pl.ds(0, PART), pl.ds(PART, PART)

    def landed(ref, sem):
        moved(ref, pair_s, sem, to_pair).wait_recv()

    def left(ref, sem):
        moved(ref, sem, pair_r, to_pair).wait_send()

    def uz(i, b, to):
        start(
            moved(up_all.at[b, y, x], uz_s, uz_r.at[i - 1], to),
            moved(taps_all.at[b], uz_s, uz_r.at[i - 1], to),
        )

    def pass_up(i):
        b = block(i)
        landed(upped.at[pl.ds(0, 40)], uz_r.at[i - 1])

        @pl.when((i < NZ - 3) & (lax.rem(i, 2) == 1))
        def _():
            uz(i + 2, b, to_zu)

        @pl.when((i < NZ - 3) & (lax.rem(i, 2) == 0))
        def _():
            uz(i + 2, b, to_zd)

        @pl.when(i == NZ - 3)
        def _():
            start(
                moved(up_all.at[b, y, x, upper], uz_s, uz_r.at[NZ - 2], to_zu),
                moved(taps_all.at[b], uz_s, uz_r.at[NZ - 2], to_zu),
            )

        @pl.when(i == NZ - 2)
        def _():
            start(moved(up_all.at[b, y, x, lower], uz_s, uz_r.at[NZ - 2], to_zd))

    def first(i, b):
        near = near_r.at[i]
        start(
            moved(up_all.at[b, y, x, upper], first_s, near, to_yu),
            moved(up_all.at[b, y, x, upper], first_s, near, to_yd),
            moved(up_all.at[b, y, x, lower], first_s, near, to_xu),
            moved(up_all.at[b, y, x, lower], first_s, near, to_xd),
        )

    def relay(i, b):
        h = PART // 2
        far = far_r.at[i]
        landed(up_all.at[b, y, pl.ds(0, 2)], near_r.at[i])
        start(
            moved(up_all.at[b, y_down, x, pl.ds(0, h)], first_s, far, to_yu),
            moved(up_all.at[b, y_up, x, pl.ds(h, h)], first_s, far, to_yd),
            moved(up_all.at[b, y, x_down, pl.ds(PART, h)], first_s, far, to_xu),
            moved(up_all.at[b, y, x_up, pl.ds(PART + h, h)], first_s, far, to_xd),
        )

    def last(i, b, p):
        there = last_r.at[i, (p + 1) // 2]
        start(
            moved(up_all.at[b, lines[p], x, upper], last_s, there, to_xu),
            moved(up_all.at[b, y, posts[p], lower], last_s, there, to_yu),
            moved(up_all.at[b, lines[p], x, upper], last_s, there, to_xd),
            moved(up_all.at[b, y, posts[p], lower], last_s, there, to_yd),
        )

    def finish(i, b):
        landed(up_all.at[b, y, x], far_r.at[i])
        last(i, b, 3)

    def hand_on(i, b, *ps):
        landed(up_all.at[b, y, pl.ds(0, 2 * len(ps))], last_r.at[i, (ps[0] + 1) // 2])
        there = last_far_r.at[i]
        for p in ps:
            px, to_x, py, to_y = (
                (x_down, to_xu, y_down, to_yu) if p < 2 else (x_up, to_xd, y_up, to_yd)
            )
            start(
                moved(up_all.at[b, lines[p], px, upper], last_s, there, to_x),
                moved(up_all.at[b, py, posts[p], lower], last_s, there, to_y),
            )

    def complete(i, b):
        landed(up_all.at[b, 0], last_far_r.at[i])

    def down_x():
        start(
            moved(down_all.at[z, y, x], dxy_s, dx_r.at[0], to_xu),
            moved(down_all.at[z, y, x], dxy_s, dx_r.at[0], to_xd),
        )

    def down_x_far():
        start(
            moved(down_all.at[z, y, x_down, pl.ds(0, 48)], dxy_s, dx_r.at[1], to_xu),
            moved(down_all.at[z, y, x_up, pl.ds(48, 48)], dxy_s, dx_r.at[1], to_xd),
        )

    def down_y(c):
        there = dy_r.at[(c + 1) // 2]
        start(
            moved(down_all.at[z, y, posts[c]], dxy_s, there, to_yu),
            moved(down_all.at[z, y, posts[c]], dxy_s, there, to_yd),
        )

    def down_y_far(c):
        there = dy_r.at[3 + (c + 1) // 2]
        start(
            moved(down_all.at[z, y_down, posts[c], pl.ds(0, 48)], dxy_s, there, to_yu),
            moved(down_all.at[z, y_up, posts[c], pl.ds(48, 48)], dxy_s, there, to_yd),
        )

    def down_z(p, *cs):
        for c in cs:
            start(
                moved(down_all.at[z, lines[p], posts[c]], dz_s, dz_r.at[0, p], to_zu),
                moved(down_all.at[z, lines[p], posts[c]], dz_s, dz_r.at[0, p], to_zd),
            )

    def down_landed(count, sem):
        landed(down_all.at[z, 0, pl.ds(0, count)], sem)

    def pass_down(s, p):
        landed(down_all.at[0, pl.ds(0, 2)], dz_r.at[s - 1, p])
        for d in (0, 1):
            b, to = block(2 * s - 1 + d), (to_zu, to_zd)[d]

            @pl.when(s < 3)
            def _():
                moved(down_all.at[b, lines[p]], dz_s, dz_r.at[s, p], to).start()

            if (p < 2) == (d == 0):
                @pl.when(s == 3)
                def _():
                    moved(down_all.at[b, lines[p]], dz_s, dz_r.at[3, 0], to).start()

    def project(b, lo, count):
        weights = up_all[b].reshape(NY * NX * 2 * PART, 3 * LANES)
        upped[lo : lo + count] = jnp.dot(
            normed[lo : lo + count], weights, preferred_element_type=jnp.float32
        )

    def down_of(b):
        half = LANES // 2
        lines_of = []
        for yy in range(NY):
            for xx in range(0, NX, 2):
                even, odd = down_all[b, yy, xx], down_all[b, yy, xx + 1]
                low = jnp.concatenate([even[:, :half], odd[:, :half]], axis=1)
                high = jnp.concatenate([even[:, half:], odd[:, half:]], axis=1)
                lines_of.append(jnp.concatenate([low, high], axis=0))
        return jnp.concatenate(lines_of, axis=1)

    def share(b, part, down):
        taps = taps_all[b]
        base = part * rows + HALO
        conv = upped[pl.ds(base - 2, rows), :] * taps[0:1]
        conv = conv + upped[pl.ds(base - 1, rows), :] * taps[1:2]
        conv = conv + upped[pl.ds(base, rows), :] * taps[2:3]
        end = conv[:, 2 * LANES :]
        main = jax.nn.gelu(conv[:, LANES : 2 * LANES], approximate=True) * conv[:, :LANES]
        rest = jax.nn.gelu(pltpu.roll(end, LANES // 2, 1), approximate=True) * end
        hidden = jnp.concatenate([main, rest], axis=1).astype(jnp.bfloat16)
        return jnp.dot(hidden[:, : down.shape[0]], down, preferred_element_type=jnp.float32)

    def compute(i):
        b = block(i)
        project(b, 0, 2 * rows + HALO)
        down = down_of(b)
        for part in (0, 1):
            total[part] += share(b, part, down)

    down_x()
    down_y(0)
    first(jnp.int32(0), z)
    uz(1, z, to_zu)
    uz(2, z, to_zd)
    down_z(0, 0)
    last(jnp.int32(0), z, 0)
    own_rows = moved(rows_all.at[core], pair_s, pair_r, to_pair)
    own_rows.start()
    edge = pltpu.make_async_remote_copy(
        src_ref=rows_all.at[1, pl.ds(rows - HALO, HALO)], dst_ref=halo, send_sem=halo_s,
        recv_sem=halo_r, device_id=to_next, device_id_type=MESH,
    )

    def normalize_rows():
        scale = norm_in_ref[...]
        for part in (0, 1):
            wide = rows_all[part].astype(jnp.float32)
            value = normalized(wide, scale).astype(jnp.bfloat16)
            normed[pl.ds(HALO + part * rows, rows), :] = value

    def normalize_halo():
        edge.wait_recv()
        origin = (y + x + z) == 0
        before = normalized(halo[...].astype(jnp.float32), norm_in_ref[...])
        normed[0:HALO] = jnp.where(origin, 0.0, before).astype(jnp.bfloat16)

    def turn(m, carry):
        n = m - 4

        @pl.when(n == -4)
        def _():
            down_landed(2, dx_r.at[0])
            down_x_far()
            down_y(1)
            down_y(2)

        @pl.when(n == -3)
        def _():
            down_landed(1, dx_r.at[1])
            down_y(3)
            down_landed(4, dy_r.at[1])
            down_y_far(1)
            down_y_far(2)

        @pl.when((n >= -3) & (n <= 0))
        def _():
            relay(2 * m - 1, block(2 * m - 1))

        @pl.when(n <= -1)
        def _():
            relay(2 * m, block(2 * m))

        @pl.when(n == -4)
        def _():
            down_landed(2, dy_r.at[0])
            down_y_far(0)

        @pl.when(n <= -1)
        def _():
            pass_up(2 * m + 1)
            first(2 * m + 1, block(2 * m + 1))

        @pl.when(n <= -2)
        def _():
            pass_up(2 * m + 2)
            first(2 * m + 2, block(2 * m + 2))

        @pl.when(n == -4)
        def _():
            down_z(0, 1, 2)
            down_z(1, 0)
            down_z(2, 0)

        @pl.when(n == -3)
        def _():
            down_z(0, 3)
            down_z(1, 1, 2)
            down_z(2, 1, 2)
            down_landed(1, dy_r.at[3])
            down_z(3, 0)

        @pl.when(n == -2)
        def _():
            down_landed(2, dy_r.at[2])
            down_y_far(3)
            down_z(1, 3)
            down_z(2, 3)
            down_landed(2, dy_r.at[4])
            down_z(3, 1, 2)

        @pl.when(n == -1)
        def _():
            down_landed(1, dy_r.at[5])
            down_z(3, 3)

        @pl.when((n >= -2) & (n < NZ - 3))
        def _():
            s = m // 2 - 1

            @pl.when(lax.rem(m, 2) == 1)
            def _():
                pass_down(s + 1, 1)
                pass_down(s + 1, 2)

            @pl.when((lax.rem(m, 2) == 0) & (n > -2))
            def _():
                pass_down(s, 3)

            @pl.when((lax.rem(m, 2) == 0) & (n < NZ - 4))
            def _():
                pass_down(s + 1, 0)

        @pl.when(n == -3)
        def _():
            finish(n + 3, block(n + 3))
            hand_on(n + 3, block(n + 3), 0)
            hand_on(n + 3, block(n + 3), 1, 2)

        @pl.when((n == -2) | (n == -1))
        def _():
            finish(2 * m - 3, block(2 * m - 3))
            finish(2 * m - 2, block(2 * m - 2))
            hand_on(n + 2, block(n + 2), 3)

        @pl.when((n >= 0) & (n + 5 < NZ))
        def _():
            finish(n + 5, block(n + 5))

        @pl.when((n >= -2) & (n + 3 < NZ))
        def _():
            hand_on(n + 3, block(n + 3), 0)
            hand_on(n + 3, block(n + 3), 1, 2)

        @pl.when((n >= -1) & (n + 3 < NZ))
        def _():
            hand_on(n + 3, block(n + 3), 3)

        @pl.when((n >= -3) & (n <= -1))
        def _():
            last(n + 4, block(n + 4), 0)

        @pl.when(n <= -1)
        def _():
            last(n + 4, block(n + 4), 1)
            last(n + 4, block(n + 4), 2)

        @pl.when((n >= -1) & (n + 5 < NZ))
        def _():
            last(n + 5, block(n + 5), 0)
            last(n + 5, block(n + 5), 1)
            last(n + 5, block(n + 5), 2)

        @pl.when(n == -4)
        def _():
            landed(rows_all.at[1 - core], pair_r)
            edge.start()
            normalize_rows()

        @pl.when(n == -2)
        def _():
            normalize_halo()

        @pl.when(n >= -1)
        def _():
            complete(n + 1, block(n + 1))
            compute(n + 1)

        return carry

    lax.fori_loop(0, NZ + 2, turn, jnp.int32(0))

    pieces = 4
    size = rows // pieces

    def piece(k):
        return pltpu.make_async_remote_copy(
            src_ref=leaving.at[k], dst_ref=arriving.at[k], send_sem=sum_s,
            recv_sem=sum_r.at[k], device_id=to_pair, device_id_type=MESH,
        )

    i = jnp.int32(NZ - 1)
    b = block(i)
    landed(down_all.at[0], dz_r.at[3, 0])
    complete(i, b)
    for mine in (0, 1):
        @pl.when(core == mine)
        def _():
            theirs = 1 - mine
            project(b, theirs * rows, rows + HALO)
            down = down_of(b)
            ready = total[theirs] + share(b, theirs, down)
            for k in range(pieces):
                leaving[k] = ready[k * size : (k + 1) * size].astype(jnp.bfloat16)
                if k:
                    piece(k - 1).start()
            project(b, mine * rows, rows + HALO)
            piece(pieces - 1).start()
            total[mine] += share(b, mine, down)

    out_scale = norm_out_ref[...]
    for k in range(pieces):
        piece(k).wait_recv()
        whole = total[core, pl.ds(k * size, size), :] + arriving[k].astype(jnp.float32)
        out_ref[pl.ds(k * size, size), :] = normalized(whole, out_scale).astype(jnp.bfloat16)

    left(up_all.at[pl.ds(0, 6), 0], first_s)
    left(up_all.at[pl.ds(0, 6)], last_s)
    left(upped.at[pl.ds(0, 280)], uz_s)
    left(down_all.at[pl.ds(0, 5), 0, pl.ds(0, 3)], dxy_s)
    left(down_all.at[pl.ds(0, 7)], dz_s)
    own_rows.wait_send()
    edge.wait_send()
    left(leaving, sum_s)


def shards(
    tokens, norm_in, value_weight, gate_weight, value_taps, gate_taps, down_weight, norm_out
):
    rows, width = tokens.shape
    bf16, f32 = jnp.bfloat16, jnp.float32
    vmem = pl.BlockSpec(memory_space=pltpu.VMEM)
    hbm = pl.BlockSpec(memory_space=pl.ANY)
    return pl.pallas_call(
        kernel,
        in_specs=[hbm, vmem, hbm, hbm, vmem, vmem, hbm, vmem],
        out_specs=vmem,
        out_shape=jax.ShapeDtypeStruct(tokens.shape, tokens.dtype),
        scratch_shapes=[
            pltpu.VMEM(value_weight.shape, bf16),
            pltpu.VMEM(value_weight.shape, bf16),
            pltpu.VMEM(down_weight.shape[::-1], bf16),
            pltpu.VMEM((NZ, NY, NX, 2 * PART, 3 * LANES), bf16),
            pltpu.VMEM((NZ, NY, NX, 96, LANES), bf16),
            pltpu.VMEM((NZ, 8, 3 * LANES), f32),
            pltpu.VMEM((2, rows, width), bf16),
            pltpu.VMEM((HALO, width), bf16),
            pltpu.VMEM((2 * rows + HALO, width), bf16),
            pltpu.VMEM((2 * rows + HALO, 3 * LANES), f32),
            pltpu.VMEM((2, rows, width), f32),
            pltpu.VMEM((4, rows // 4, width), bf16),
            pltpu.VMEM((4, rows // 4, width), bf16),
        ]
        + [DMA] * 5
        + [DMA((NZ - 1,))]
        + [DMA((NZ,))] * 2
        + [DMA((NZ, 3)), DMA((NZ,))]
        + [DMA((2,)), DMA((6,))]
        + [DMA((4, 4)), DMA((4,))]
        + [DMA] * 5
        + [DMA((4,))],
        compiler_params=pltpu.CompilerParams(
            collective_id=0, has_side_effects=True, vmem_limit_bytes=56 * 2**20
        ),
    )(
        tokens, norm_in[None], value_weight, gate_weight, value_taps, gate_taps, down_weight.T,
        norm_out[None],
    )


def solution(mesh):
    split = Mesh(mesh.devices.reshape(NY, NX, NZ, 2), ALL)
    return jax.shard_map(
        shards,
        mesh=split,
        in_specs=(
            P(ALL, None),
            P(),
            P(FS, ("z", "core")),
            P(FS, ("z", "core")),
            P(None, ("z", "core")),
            P(None, ("z", "core")),
            P(("z", "core"), FS),
            P(),
        ),
        out_specs=P(ALL, None),
        check_vma=False,
    )
```
